256 devices in a mesh: ep: 32 (over z, x), tp: 8 (over y, core).
Axes of the slice: x: 4, y: 4, z: 8, core: 2. Of those that a mesh axis runs over, the one named last changes fastest.
Arguments:
- tokens: bfloat16 [32768, 2048], P(('ep', 'tp')), may hold values from -24 to 24
- expert_ids: int32 [32768, 4], P(('ep', 'tp')), may hold values from 0 to 31, all different within a row; in each aligned block of 128 rows (0 to 127, 128 to 255, ...) at most 24 rows name the same one
- route_weights: float32 [32768, 4], P(('ep', 'tp')), may hold values from 0.2 to 1.2
- cotangent: bfloat16 [32768, 2048], P(('ep', 'tp')), may hold values from -24 to 24
- gate_weight: bfloat16 [256, 512, 2048], P(('ep', 'tp')), may hold values from -0.125 to 0.125
- up_weight: bfloat16 [256, 512, 2048], P(('ep', 'tp')), may hold values from -0.125 to 0.125
- down_weight: bfloat16 [256, 512, 2048], P(('ep', 'tp')), may hold values from -0.25 to 0.25
- shared_gate: bfloat16 [256, 2048], replicated, may hold values from -0.125 to 0.125
- shared_up: bfloat16 [256, 2048], replicated, may hold values from -0.125 to 0.125
- shared_down: bfloat16 [256, 2048], replicated, may hold values from -0.375 to 0.375
Outputs:
- token_grad: bfloat16 [32768, 2048], P(('ep', 'tp'))
- route_grad: float32 [32768, 4], P(('ep', 'tp'))
- gate_grad: bfloat16 [256, 512, 2048], P(('ep', 'tp'))
- up_grad: bfloat16 [256, 512, 2048], P(('ep', 'tp'))
- down_grad: bfloat16 [256, 512, 2048], P(('ep', 'tp'))
- shared_grads: float32 [2048, 3, 256], P(('ep', 'tp'))
The draws below stay inside these ranges and needn't reach their ends.
Inputs may be any that keep to these rules, and one draw needn't show every extreme that they name: `expert_ids`: each row names 4 different numbers of 0 to 31, experts within the group of the row's device. Among the rows of one device (aligned blocks of 128 tokens) no number is named more than 24 times, and in some blocks one number is named exactly 24 times.
All inputs are finite; a program needn't handle non-finite values.
Results may differ from the reference program's by a relative error of at most 0.006.
Values may be sent and summed in bfloat16 or wider, within the bound.
A program may use at most 128 MiB of HBM per device.

```python
import math
import jax
import jax.numpy as jnp
import numpy as np
from jax import lax

D = 2048
D_EXPERT = 512
D_SHARED = 256
TOP = 4
TOK_DEV = 128
GROUPS = 8
EXP_GROUP = 32
EXPERTS = 256
CAP = 24
TOKENS = 32768


def with_spikes(array, key, source, target, shards_of, factor):
    owner, partner = [(jnp.arange(array.shape[dim]) // (array.shape[dim] // shards_of)).reshape([-1 if axis == dim else 1 for axis in range(array.ndim)]) for dim in (source, target)]
    chosen = jax.random.permutation(key, shards_of)[partner]
    strong = (owner == chosen) | (owner == (partner + shards_of // 2) % shards_of)
    return jnp.where(strong, factor * array, array)


def level_of(key, extent, cuts, smallest, high):
    factor_of = 1.0
    for axis_at, parts in cuts:
        heights = jax.random.uniform(jax.random.fold_in(jax.random.fold_in(key, 6), axis_at), (parts,), jnp.float32, smallest / len(cuts), high / len(cuts))
        factor_of = factor_of * jnp.repeat(jnp.exp(heights), extent[axis_at] // parts).reshape((-1,) + (1,) * (len(extent) - 1 - axis_at))
    return factor_of


def routed_block(stream_key, own, number, rows, amount, top, most, skew):
    sequence = jax.random.permutation(stream_key, amount)
    packed, usual = load_shares(amount, rows * top, most, skew, True), load_shares(amount, rows * top, most, skew, False)
    places = jnp.arange(amount)

    def named(sizes, turn):
        used = int((sizes > 0).sum())
        fixed = max(1, used // 4)
        shifted = fixed + (places - fixed + turn * (used - fixed)) % max(1, amount - fixed)
        return jnp.zeros((amount,), jnp.int32).at[sequence[jnp.where(places < fixed, places, shifted)]].set(jnp.asarray(sizes, jnp.int32))

    sizes = jnp.where(number % 4 == 0, named(packed, number // 4), named(usual, number - number // 4 - 1))
    mixed = jax.random.permutation(jax.random.fold_in(own, 3), amount)
    giver, taker = mixed[0:amount // 2 * 2:2], mixed[1:amount // 2 * 2:2]
    slack = jnp.minimum(sizes[giver] - 1, most - sizes[taker]) // 2
    slack = jnp.where((giver == sequence[0]) | (taker == sequence[0]) | (sizes[taker] == 0), 0, jnp.maximum(slack, 0))
    shifted = jax.random.randint(jax.random.fold_in(own, 4), (amount // 2,), 0, 1 << 20) % (slack + 1)
    sizes = sizes.at[giver].add(-shifted).at[taker].add(shifted)
    labels = jnp.searchsorted(jnp.cumsum(sizes), jnp.arange(rows * top), side="right").astype(jnp.int32)
    listing = labels.reshape(top, rows).T
    listing = listing[jax.random.permutation(jax.random.fold_in(own, 1), rows)]
    turn = jax.random.randint(jax.random.fold_in(own, 2), (rows, 1), 0, top)
    return jnp.take_along_axis(listing, (jnp.arange(top)[None, :] + turn) % top, axis=1)


def load_shares(count, total, bound, lean, full):
    weights = [(1 << 20) // math.isqrt(grade ** lean) + 1 for grade in range(1, count + 1)]
    largest = bound if full else min(bound, max(-(-total // count), total * weights[0] // sum(weights)))
    least = 1 if total - largest >= count - 1 else 0
    given, surplus = [largest] + [least] * (count - 1), total - largest - least * (count - 1)
    while surplus > 0:
        free = [i for i in range(1, count) if given[i] < largest] or [i for i in range(1, count) if given[i] < bound]
        whole, budget = sum([weights[i] for i in free]), surplus
        for i in free:
            more = min(bound - given[i], max(1, budget * weights[i] // whole), surplus)
            given[i] = given[i] + more
            surplus = surplus - more
    return np.array(given)


def gaussian(own_key, dims, spread, most, pieces=(), kind=jnp.bfloat16):
    drawn = jax.random.normal(own_key, dims, jnp.float32) * spread
    if len(pieces) > 0:
        drawn = level_of(own_key, dims, pieces, -0.22, 0.18) * drawn
    return jnp.clip(drawn, min=-most, max=most).astype(kind)


def gaussian_with(rng, dims, width, most, pieces, heavy, held_as=jnp.bfloat16):
    values = width * jax.random.normal(rng, dims, jnp.float32)
    if pieces:
        values = values * level_of(rng, dims, pieces, -0.22, 0.18)
    return jnp.clip(with_spikes(values, jax.random.fold_in(rng, 3), *heavy), -most, most).astype(held_as)


def setup_inputs(seed: int = 0) -> dict:
    key_of = jax.random.split(jax.random.key(seed), 11)
    tokens = gaussian_with(key_of[0], (TOKENS, D), 1.0, 24.0, ((0, 256),), (0, 1, 256, 6.0))
    expert_ids_keys = jax.random.split(jax.random.fold_in(key_of[1], 1), TOKENS // TOK_DEV)
    expert_ids_turns = jax.random.permutation(jax.random.fold_in(key_of[1], 3), TOKENS // TOK_DEV)
    expert_ids = jax.vmap(lambda own, number: routed_block(jax.random.fold_in(key_of[1], 2), own, number, TOK_DEV, EXP_GROUP, TOP, CAP, 2))(expert_ids_keys, expert_ids_turns).reshape((TOKENS, TOP))
    route_weights = jnp.clip(0.2 + 1 * jax.random.uniform(key_of[2], (TOKENS, TOP), jnp.float32) ** level_of(key_of[2], (TOKENS, TOP), ((0, 256),), -0.2, 0.2), 0.2, 1.2)
    cotangent = gaussian_with(key_of[3], (TOKENS, D), 1.0, 24.0, ((0, 256),), (0, 1, 256, 6.0))
    gate_weight = gaussian(key_of[4], (EXPERTS, D_EXPERT, D), D ** -0.5, 0.125, ((0, 256),))
    up_weight = gaussian(key_of[5], (EXPERTS, D_EXPERT, D), D ** -0.5, 0.125, ((0, 256),))
    down_weight = gaussian(key_of[6], (EXPERTS, D_EXPERT, D), D_EXPERT ** -0.5, 0.25, ((0, 256),))
    shared_gate = gaussian(key_of[7], (D_SHARED, D), D ** -0.5, 0.125)
    shared_up = gaussian(key_of[8], (D_SHARED, D), D ** -0.5, 0.125)
    shared_down = gaussian(key_of[9], (D_SHARED, D), D_SHARED ** -0.5, 0.375)
    return dict(tokens=tokens, expert_ids=expert_ids, route_weights=route_weights, cotangent=cotangent, gate_weight=gate_weight, up_weight=up_weight, down_weight=down_weight, shared_gate=shared_gate, shared_up=shared_up, shared_down=shared_down)


def gated_backward(scaled, gate_pre, up_pre):
    sigmoid_gate = jax.nn.sigmoid(gate_pre)
    gate_delta = (scaled * up_pre * sigmoid_gate * (1.0 + gate_pre * (1.0 - sigmoid_gate))).astype(jnp.bfloat16)
    up_delta = (scaled * jax.nn.silu(gate_pre)).astype(jnp.bfloat16)
    return gate_delta, up_delta


def slots_of(block_ids):
    one_hot = (block_ids[:, None] == jnp.arange(EXP_GROUP, dtype=jnp.int32)[None, :]).astype(jnp.int32)
    return (jnp.sum(jnp.cumsum(one_hot, axis=0) * one_hot, axis=1) - 1).astype(jnp.int32)


def reference(tokens, expert_ids, route_weights, cotangent, gate_weight, up_weight, down_weight, shared_gate, shared_up, shared_down):
    blocks = TOKENS // TOK_DEV
    local_ids = expert_ids.reshape(blocks, TOK_DEV * TOP).astype(jnp.int32)
    slot_index = jax.vmap(slots_of)(local_ids)
    block_index = jnp.arange(blocks, dtype=jnp.int32)[:, None]
    group_index = block_index % GROUPS
    source_index = block_index // GROUPS
    expert_index = local_ids * GROUPS + group_index
    position = ((expert_index * EXP_GROUP + source_index) * CAP + slot_index).reshape(-1).astype(jnp.int32)
    assign_count = TOKENS * TOP
    rows_each = EXP_GROUP * CAP
    slots_all = EXPERTS * rows_each
    row_assign = jnp.full((slots_all,), assign_count, jnp.int32).at[position].set(jnp.arange(assign_count, dtype=jnp.int32))
    empty_row = jnp.zeros((1, D), jnp.bfloat16)
    padded_tokens = jnp.concatenate([tokens, empty_row], axis=0)
    padded_cot = jnp.concatenate([cotangent, empty_row], axis=0)
    padded_weights = jnp.concatenate([route_weights.reshape(-1), jnp.zeros((1,), jnp.float32)], axis=0)

    def expert_step(carry, inputs):
        token_acc, route_acc = carry
        gate_w, up_w, down_w, assign = inputs
        row_ids = (assign // TOP).astype(jnp.int32)
        weights = jnp.take(padded_weights, assign, axis=0)
        token_rows = jnp.take(padded_tokens, row_ids, axis=0)
        cot_rows = jnp.take(padded_cot, row_ids, axis=0)
        gate_pre = jnp.dot(token_rows, gate_w.T, preferred_element_type=jnp.float32)
        up_pre = jnp.dot(token_rows, up_w.T, preferred_element_type=jnp.float32)
        hidden = (jax.nn.silu(gate_pre) * up_pre).astype(jnp.bfloat16)
        back_hidden = jnp.dot(cot_rows, down_w.T, preferred_element_type=jnp.float32)
        route_part = jnp.sum(back_hidden * hidden.astype(jnp.float32), axis=1)
        gate_delta, up_delta = gated_backward(weights[:, None] * back_hidden, gate_pre, up_pre)
        weighted_cot = (weights[:, None] * cot_rows.astype(jnp.float32)).astype(jnp.bfloat16)
        token_part = jnp.dot(gate_delta, gate_w, preferred_element_type=jnp.float32) + jnp.dot(up_delta, up_w, preferred_element_type=jnp.float32)
        grad_gate = jnp.dot(gate_delta.T, token_rows, preferred_element_type=jnp.float32).astype(jnp.bfloat16)
        grad_up = jnp.dot(up_delta.T, token_rows, preferred_element_type=jnp.float32).astype(jnp.bfloat16)
        grad_down = jnp.dot(hidden.T, weighted_cot, preferred_element_type=jnp.float32).astype(jnp.bfloat16)
        token_acc = token_acc.at[row_ids].add(token_part)
        route_acc = route_acc.at[assign].set(route_part)
        return (token_acc, route_acc), (grad_gate, grad_up, grad_down)

    start = (jnp.zeros((TOKENS + 1, D), jnp.float32), jnp.zeros((assign_count + 1,), jnp.float32))
    (token_acc, route_acc), (gate_grad, up_grad, down_grad) = lax.scan(
        expert_step, start, (gate_weight, up_weight, down_weight, row_assign.reshape(EXPERTS, rows_each)))
    routed = token_acc[:TOKENS]
    route_grad = route_acc[:assign_count].reshape(TOKENS, TOP)

    common_gate = jnp.dot(tokens, shared_gate.T, preferred_element_type=jnp.float32)
    common_up = jnp.dot(tokens, shared_up.T, preferred_element_type=jnp.float32)
    common_hidden = (jax.nn.silu(common_gate) * common_up).astype(jnp.bfloat16)
    common_back = jnp.dot(cotangent, shared_down.T, preferred_element_type=jnp.float32)
    common_gate_delta, common_up_delta = gated_backward(common_back, common_gate, common_up)
    common_part = jnp.dot(common_gate_delta, shared_gate, preferred_element_type=jnp.float32) + jnp.dot(common_up_delta, shared_up, preferred_element_type=jnp.float32)
    shared_grads = jnp.stack([
        jnp.dot(tokens.T, common_gate_delta, preferred_element_type=jnp.float32),
        jnp.dot(tokens.T, common_up_delta, preferred_element_type=jnp.float32),
        jnp.dot(cotangent.T, common_hidden, preferred_element_type=jnp.float32)], axis=1)
    token_grad = (routed + common_part).astype(jnp.bfloat16)
    return (token_grad, route_grad, gate_grad, up_grad, down_grad, shared_grads)
```

```python
import jax
import jax.numpy as jnp
from jax import lax
from jax.sharding import PartitionSpec as P


def gated_backward(scaled, gate_pre, up_pre):
    sigmoid_gate = jax.nn.sigmoid(gate_pre)
    gate_delta = (scaled * up_pre * sigmoid_gate * (1.0 + gate_pre * (1.0 - sigmoid_gate))).astype(
        jnp.bfloat16
    )
    up_delta = (scaled * jax.nn.silu(gate_pre)).astype(jnp.bfloat16)
    return (gate_delta, up_delta)


def forward_products(token_rows, gate_local, up_local):
    gate_pre = jnp.einsum("rd,fd->rf", token_rows, gate_local, preferred_element_type=jnp.float32)
    up_pre = jnp.einsum("rd,fd->rf", token_rows, up_local, preferred_element_type=jnp.float32)
    return (gate_pre, up_pre)


def shards(
    tokens,
    expert_ids,
    route_weights,
    cotangent,
    gate_weight,
    up_weight,
    down_weight,
    shared_gate,
    shared_up,
    shared_down,
):
    ep_size = lax.axis_size("ep")
    tok_rows = tokens.shape[0]
    model_width = tokens.shape[1]
    top_count = expert_ids.shape[1]
    capacity = 3 * tok_rows * top_count // (2 * ep_size)
    slots_all = ep_size * capacity
    assign_count = tok_rows * top_count
    flat_ids = expert_ids.reshape(-1)
    one_hot = (flat_ids[:, None] == jnp.arange(ep_size, dtype=jnp.int32)[None, :]).astype(jnp.int32)
    slot_index = jnp.sum(jnp.cumsum(one_hot, axis=0) * one_hot, axis=1) - 1
    position = flat_ids * capacity + slot_index
    row_assign = (
        jnp.full((slots_all,), assign_count, jnp.int32)
        .at[position]
        .set(jnp.arange(assign_count, dtype=jnp.int32))
    )
    row_token = row_assign // top_count
    row_weight = jnp.take(
        jnp.concatenate([route_weights.reshape(-1), jnp.zeros((1,), jnp.float32)], axis=0),
        row_assign,
        axis=0,
    )
    empty_row = jnp.zeros((1, model_width), jnp.bfloat16)
    send_tokens = jnp.take(jnp.concatenate([tokens, empty_row], axis=0), row_token, axis=0).reshape(
        ep_size, capacity, model_width
    )
    send_cot = jnp.take(jnp.concatenate([cotangent, empty_row], axis=0), row_token, axis=0).reshape(
        ep_size, capacity, model_width
    )
    gate_local = gate_weight[0]
    up_local = up_weight[0]
    down_local = down_weight[0]
    scales = lax.all_to_all(
        row_weight.reshape(ep_size, capacity), "ep", split_axis=0, concat_axis=0, tiled=True
    ).reshape(slots_all)
    token_rows, cot_rows = (
        lax.all_to_all(send_tokens, "ep", split_axis=0, concat_axis=0, tiled=True),
        lax.all_to_all(send_cot, "ep", split_axis=0, concat_axis=0, tiled=True),
    )
    token_rows = token_rows.reshape(slots_all, model_width)
    cot_rows = cot_rows.reshape(slots_all, model_width)
    gate_pre, up_pre = forward_products(token_rows, gate_local, up_local)
    hidden = (jax.nn.silu(gate_pre) * up_pre).astype(jnp.bfloat16)
    back_hidden = jnp.einsum("rd,fd->rf", cot_rows, down_local, preferred_element_type=jnp.float32)
    route_part = jnp.sum(back_hidden * hidden.astype(jnp.float32), axis=1)
    gate_delta, up_delta = gated_backward(scales[:, None] * back_hidden, gate_pre, up_pre)
    weighted_cot = (scales[:, None] * cot_rows.astype(jnp.float32)).astype(jnp.bfloat16)
    token_part = jnp.einsum(
        "rf,fd->rd", gate_delta, gate_local, preferred_element_type=jnp.float32
    ) + jnp.einsum("rf,fd->rd", up_delta, up_local, preferred_element_type=jnp.float32)
    gate_grad = jnp.einsum(
        "rf,rd->fd", gate_delta, token_rows, preferred_element_type=jnp.float32
    ).astype(jnp.bfloat16)[None]
    up_grad = jnp.einsum(
        "rf,rd->fd", up_delta, token_rows, preferred_element_type=jnp.float32
    ).astype(jnp.bfloat16)[None]
    down_grad = jnp.einsum(
        "rf,rd->fd", hidden, weighted_cot, preferred_element_type=jnp.float32
    ).astype(jnp.bfloat16)[None]
    back_rows, back_route = (
        lax.all_to_all(
            token_part.astype(jnp.bfloat16).reshape(ep_size, capacity, model_width),
            "ep",
            split_axis=0,
            concat_axis=0,
            tiled=True,
        ),
        lax.all_to_all(
            route_part.reshape(ep_size, capacity), "ep", split_axis=0, concat_axis=0, tiled=True
        ),
    )
    routed = jnp.sum(
        jnp.take(back_rows.reshape(slots_all, model_width), position, axis=0)
        .reshape(tok_rows, top_count, model_width)
        .astype(jnp.float32),
        axis=1,
    )
    route_grad = jnp.take(back_route.reshape(slots_all), position, axis=0).reshape(
        tok_rows, top_count
    )
    common_gate = jnp.einsum("td,fd->tf", tokens, shared_gate, preferred_element_type=jnp.float32)
    common_up = jnp.einsum("td,fd->tf", tokens, shared_up, preferred_element_type=jnp.float32)
    common_hidden = (jax.nn.silu(common_gate) * common_up).astype(jnp.bfloat16)
    common_back = jnp.einsum(
        "td,fd->tf", cotangent, shared_down, preferred_element_type=jnp.float32
    )
    common_gate_delta, common_up_delta = gated_backward(common_back, common_gate, common_up)
    common_part = jnp.einsum(
        "tf,fd->td", common_gate_delta, shared_gate, preferred_element_type=jnp.float32
    ) + jnp.einsum("tf,fd->td", common_up_delta, shared_up, preferred_element_type=jnp.float32)
    partial = jnp.stack(
        [
            jnp.einsum("tc,tf->cf", tokens, common_gate_delta, preferred_element_type=jnp.float32),
            jnp.einsum("tc,tf->cf", tokens, common_up_delta, preferred_element_type=jnp.float32),
            jnp.einsum("tc,tf->cf", cotangent, common_hidden, preferred_element_type=jnp.float32),
        ],
        axis=1,
    ).astype(jnp.bfloat16)
    tp_size = lax.axis_size("tp")
    partial = partial.reshape(ep_size, tp_size, -1, 768).transpose(1, 0, 2, 3)
    partial = lax.all_to_all(partial, "tp", split_axis=0, concat_axis=0, tiled=True)
    partial = jnp.sum(partial.astype(jnp.float32), axis=0)
    partial = lax.all_to_all(partial, "ep", split_axis=0, concat_axis=0, tiled=True)
    shared_grads = jnp.sum(partial, axis=0).reshape(-1, 3, 256)
    token_grad = (routed + common_part).astype(jnp.bfloat16)
    return (token_grad, route_grad, gate_grad, up_grad, down_grad, shared_grads)


def solution(mesh):
    in_specs = (
        P(("ep", "tp"), None),
        P(("ep", "tp"), None),
        P(("ep", "tp"), None),
        P(("ep", "tp"), None),
        P(("ep", "tp"), None, None),
        P(("ep", "tp"), None, None),
        P(("ep", "tp"), None, None),
        P(),
        P(),
        P(),
    )
    out_specs = (
        P(("ep", "tp"), None),
        P(("ep", "tp"), None),
        P(("ep", "tp"), None, None),
        P(("ep", "tp"), None, None),
        P(("ep", "tp"), None, None),
        P(("ep", "tp"), None, None),
    )
    return jax.shard_map(shards, mesh=mesh, in_specs=in_specs, out_specs=out_specs, check_vma=False)
```
